32 devices in a mesh: sp: 8 (over z, x), tp: 4 (over y, core).
Axes of the slice: x: 2, y: 2, z: 4, core: 2. Of those that a mesh axis runs over, the one named last changes fastest.
Arguments:
- saved_tokens: bfloat16 [1536, 2048], P('sp'), may hold values from -3.75 to 3.75
- cotangent: bfloat16 [1536, 2048], P('sp'), may hold values from -6 to 6
- routes: int32 [1536, 2], P('sp'), may hold values from 0 to 7, all different within a row; in each aligned block of 192 rows (0 to 191, 192 to 383, ...) at most 96 rows name the same one
- route_weights: float32 [1536, 2], P('sp'), may hold values from 0.2 to 1
- gate_in: bfloat16 [1536, 1024], P('sp', 'tp'), may hold values from -6 to 6
- conv_in: bfloat16 [1536, 1024], P('sp', 'tp'), may hold values from -6 to 6
- value_in: bfloat16 [1536, 1024], P('sp', 'tp'), may hold values from -6 to 6
- conv_taps: float32 [3, 1024], replicated, may hold values from -3.5 to 3.5
- out_weight: bfloat16 [2048, 1024], P(None, 'tp'), may hold values from -0.1875 to 0.1875
- gate_proj: bfloat16 [8, 2048, 2048], P('sp', None, 'tp'), may hold values from -0.125 to 0.125
- up_proj: bfloat16 [8, 2048, 2048], P('sp', None, 'tp'), may hold values from -0.125 to 0.125
- down_proj: bfloat16 [8, 2048, 2048], P('sp', 'tp'), may hold values from -0.125 to 0.125
Outputs:
- gate_proj_grad: float32 [8, 2048, 2048], P('sp', None, 'tp')
- up_proj_grad: float32 [8, 2048, 2048], P('sp', None, 'tp')
- down_proj_grad: float32 [8, 2048, 2048], P('sp', 'tp')
- out_weight_grad: float32 [2048, 1024], P('sp', 'tp')
- token_grad: bfloat16 [1536, 2048], P('sp', 'tp')
- gate_in_grad: bfloat16 [1536, 1024], P('sp', 'tp')
- conv_in_grad: bfloat16 [1536, 1024], P('sp', 'tp')
- value_in_grad: bfloat16 [1536, 1024], P('sp', 'tp')
The draws below stay inside these ranges and needn't reach their ends.
Inputs may be any that keep to these rules, and one draw needn't show every extreme that they name: `routes`: within each aligned block of 192 tokens at most 96 assignments name one expert, a bound that some block reaches of them; the 2 experts of a token differ.
All inputs are finite; a program needn't handle non-finite values.
Results may differ from the reference program's by a relative error of at most 0.0063.
Values may be sent and summed in bfloat16 or wider, within the bound.
A program may use at most 64 MiB of HBM per device.

```python
import math
import jax
import jax.numpy as jnp
import numpy as np
from jax import lax

D = 2048
FF = 2048
DC = 1024
TAPS = 3
TOP = 2
TOK_DEV = 192
EXPERTS = 8
TOKENS = 1536
CAP = 96
HID_GROUPS = 4
N_SP = 8


def spiked(drawn, stream_key, source, target, shards_of, factor):
    def block_of(axis_at):
        return (jnp.arange(drawn.shape[axis_at]) // (drawn.shape[axis_at] // shards_of)).reshape((-1,) + (1,) * (drawn.ndim - 1 - axis_at))

    first = jax.random.permutation(stream_key, shards_of)[block_of(target)]
    far = (block_of(target) + shards_of // 2) % shards_of
    return jnp.where((block_of(source) == first) | (block_of(source) == far), factor * drawn, drawn)


def steps_of(own_key, dims, shards, low, largest):
    def one(position, shards_of):
        draws = jax.random.uniform(jax.random.fold_in(jax.random.fold_in(own_key, 6), position), (shards_of,), jnp.float32, low / len(shards), largest / len(shards))
        return jnp.repeat(jnp.exp(draws), dims[position] // shards_of).reshape((-1,) + (1,) * (len(dims) - position - 1))

    gain = one(*shards[0])
    for cut in shards[1:]:
        gain = gain * one(*cut)
    return gain


def routed_block(rng, own, number, rows, number_of, top, most, skew):
    sequence = jax.random.permutation(rng, number_of)
    crowded, ordinary = load_shares(number_of, rows * top, most, skew, True), load_shares(number_of, rows * top, most, skew, False)
    places = jnp.arange(number_of)

    def named(lengths, offset_by):
        used = int((lengths > 0).sum())
        fixed = max(1, used // 4)
        shifted = fixed + (places - fixed + offset_by * (used - fixed)) % max(1, number_of - fixed)
        return jnp.zeros((number_of,), jnp.int32).at[sequence[jnp.where(places < fixed, places, shifted)]].set(jnp.asarray(lengths, jnp.int32))

    lengths = jnp.where(number % 4 == 0, named(crowded, number // 4), named(ordinary, number - number // 4 - 1))
    mixed = jax.random.permutation(jax.random.fold_in(own, 3), number_of)
    source_of, taker = mixed[0:number_of // 2 * 2:2], mixed[1:number_of // 2 * 2:2]
    room = jnp.minimum(lengths[source_of] - 1, most - lengths[taker]) // 2
    room = jnp.where((source_of == sequence[0]) | (taker == sequence[0]) | (lengths[taker] == 0), 0, jnp.maximum(room, 0))
    shifted = jax.random.randint(jax.random.fold_in(own, 4), (number_of // 2,), 0, 1 << 20) % (room + 1)
    lengths = lengths.at[source_of].add(-shifted).at[taker].add(shifted)
    items = jnp.searchsorted(jnp.cumsum(lengths), jnp.arange(rows * top), side="right").astype(jnp.int32)
    table = items.reshape(top, rows).T
    table = table[jax.random.permutation(jax.random.fold_in(own, 1), rows)]
    offset_by = jax.random.randint(jax.random.fold_in(own, 2), (rows, 1), 0, top)
    return jnp.take_along_axis(table, (jnp.arange(top)[None, :] + offset_by) % top, axis=1)


def load_shares(number_of, total, most, lean, full):
    portions = [(1 << 20) // math.isqrt(rank ** lean) + 1 for rank in range(1, number_of + 1)]
    largest = most if full else min(most, max(-(-total // number_of), total * portions[0] // sum(portions)))
    least = 1 if total - largest >= number_of - 1 else 0
    holding, spare = [largest] + [least] * (number_of - 1), total - largest - least * (number_of - 1)
    while spare > 0:
        free = [i for i in range(1, number_of) if holding[i] < largest] or [i for i in range(1, number_of) if holding[i] < most]
        pool, budget = sum([portions[i] for i in free]), spare
        for i in free:
            more = min(most - holding[i], max(1, budget * portions[i] // pool), spare)
            holding[i] = holding[i] + more
            spare = spare - more
    return np.array(holding)


def bell_draw(own_key, extent, scale, most, shards=(), kind=jnp.bfloat16):
    array = scale * jax.random.normal(own_key, extent, jnp.float32)
    if shards:
        array = array * steps_of(own_key, extent, shards, -0.22, 0.18)
    return jnp.clip(array, -most, most).astype(kind)


def gaussian_with(stream_key, extent, scale, most, pieces, heavy, kind=jnp.bfloat16):
    values = scale * jax.random.normal(stream_key, extent, jnp.float32)
    if pieces:
        values = values * steps_of(stream_key, extent, pieces, -0.22, 0.18)
    return jnp.clip(spiked(values, jax.random.fold_in(stream_key, 3), *heavy), -most, most).astype(kind)


def setup_inputs(seed: int = 0) -> dict:
    splits = jax.random.split(jax.random.key(seed), 13)
    saved_tokens = bell_draw(splits[0], (TOKENS, D), 1.25, 3.75, ((0, 8),))
    cotangent = gaussian_with(splits[1], (TOKENS, D), 1.0, 6.0, ((0, 8),), (0, 1, 8, 2.0))
    routes_keys = jax.random.split(jax.random.fold_in(splits[2], 1), TOKENS // TOK_DEV)
    routes_turns = jax.random.permutation(jax.random.fold_in(splits[2], 3), TOKENS // TOK_DEV)
    routes = jax.vmap(lambda own, number: routed_block(jax.random.fold_in(splits[2], 2), own, number, TOK_DEV, EXPERTS, TOP, CAP, 1))(routes_keys, routes_turns).reshape((TOKENS, TOP))
    route_weights = jnp.clip(0.2 + 0.8 * jax.random.uniform(splits[3], (TOKENS, TOP), jnp.float32) ** steps_of(splits[3], (TOKENS, TOP), ((0, 8),), -0.2, 0.2), 0.2, 1.0)
    gate_in = bell_draw(splits[4], (TOKENS, DC), 1.0, 6.0, ((0, 8), (1, 4)))
    conv_in = bell_draw(splits[5], (TOKENS, DC), 1.0, 6.0, ((0, 8), (1, 4)))
    value_in = bell_draw(splits[6], (TOKENS, DC), 1.0, 6.0, ((0, 8), (1, 4)))
    conv_taps = bell_draw(splits[7], (TAPS, DC), TAPS ** -0.5, 3.5, (), jnp.float32)
    out_weight = bell_draw(splits[8], (D, DC), DC ** -0.5, 0.1875, ((1, 4),))
    gate_proj = bell_draw(splits[9], (EXPERTS, D, FF), D ** -0.5, 0.125, ((0, 8), (2, 4)))
    up_proj = bell_draw(splits[10], (EXPERTS, D, FF), D ** -0.5, 0.125, ((0, 8), (2, 4)))
    down_proj = bell_draw(splits[11], (EXPERTS, FF, D), FF ** -0.5, 0.125, ((0, 8), (1, 4)))
    return dict(saved_tokens=saved_tokens, cotangent=cotangent, routes=routes, route_weights=route_weights, gate_in=gate_in, conv_in=conv_in, value_in=value_in, conv_taps=conv_taps, out_weight=out_weight, gate_proj=gate_proj, up_proj=up_proj, down_proj=down_proj)


CLAMP_LIMIT = 7.0
SILU_ALPHA = 1.702


def expert_pass(members):
    rows_in, grads_in, w_gate, w_up, w_down = members
    gate_pre = jnp.dot(rows_in, w_gate, preferred_element_type=jnp.float32)
    up_pre = jnp.dot(rows_in, w_up, preferred_element_type=jnp.float32)
    gate_clip = jnp.minimum(gate_pre, CLAMP_LIMIT)
    up_clip = jnp.clip(up_pre, -CLAMP_LIMIT, CLAMP_LIMIT)
    sigmoid_gate = jax.nn.sigmoid(SILU_ALPHA * gate_clip)
    gated_act = gate_clip * sigmoid_gate
    hidden = ((up_clip + 1.0) * gated_act).astype(jnp.bfloat16)
    d_hidden = jnp.dot(grads_in, w_down.T, preferred_element_type=jnp.float32)
    d_up = jnp.where(jnp.abs(up_pre) < CLAMP_LIMIT, d_hidden * gated_act, 0.0).astype(jnp.bfloat16)
    gate_slope = sigmoid_gate + SILU_ALPHA * gate_clip * sigmoid_gate * (1.0 - sigmoid_gate)
    d_gate = jnp.where(gate_pre < CLAMP_LIMIT, d_hidden * (up_clip + 1.0) * gate_slope, 0.0).astype(jnp.bfloat16)
    down_grad = jnp.dot(hidden.T, grads_in, preferred_element_type=jnp.float32)
    gate_grad = jnp.dot(rows_in.T, d_gate, preferred_element_type=jnp.float32)
    up_grad = jnp.dot(rows_in.T, d_up, preferred_element_type=jnp.float32)
    group_width = FF // HID_GROUPS
    slot_count = rows_in.shape[0]
    gate_terms = jnp.einsum('rgf,dgf->grd',
                            d_gate.astype(jnp.float32).reshape(slot_count, HID_GROUPS, group_width),
                            w_gate.astype(jnp.float32).reshape(D, HID_GROUPS, group_width))
    up_terms = jnp.einsum('rgf,dgf->grd',
                          d_up.astype(jnp.float32).reshape(slot_count, HID_GROUPS, group_width),
                          w_up.astype(jnp.float32).reshape(D, HID_GROUPS, group_width))
    rounded = lax.optimization_barrier((gate_terms + up_terms).astype(jnp.bfloat16))
    return gate_grad, up_grad, down_grad, jnp.sum(rounded.astype(jnp.float32), axis=0)


def reference(saved_tokens, cotangent, routes, route_weights, gate_in, conv_in, value_in,
              conv_taps, out_weight, gate_proj, up_proj, down_proj):
    block_assigns = TOK_DEV * TOP
    flat_routes = routes.reshape(N_SP, block_assigns).astype(jnp.int32)
    onehot = (flat_routes[:, :, None] == jnp.arange(EXPERTS, dtype=jnp.int32)[None, None, :]).astype(jnp.int32)
    slot_rank = jnp.sum((jnp.cumsum(onehot, axis=1) - 1) * onehot, axis=2)
    source = jnp.arange(N_SP, dtype=jnp.int32)[:, None]
    slot_index = (flat_routes * (N_SP * CAP) + source * CAP + slot_rank).reshape(-1).astype(jnp.int32)
    total_assigns = TOKENS * TOP
    slot_owner = jnp.full((EXPERTS * N_SP * CAP,), total_assigns, jnp.int32).at[slot_index].set(
        jnp.arange(total_assigns, dtype=jnp.int32))
    zero_row = jnp.zeros((1, D), jnp.bfloat16)
    token_rows = jnp.concatenate([saved_tokens, zero_row], 0)[slot_owner // TOP].reshape(EXPERTS, N_SP * CAP, D)
    scaled = (route_weights[:, :, None] * cotangent.astype(jnp.float32)[:, None, :]).astype(jnp.bfloat16)
    scaled = scaled.reshape(total_assigns, D)
    grad_rows = jnp.concatenate([scaled, zero_row], 0)[slot_owner].reshape(EXPERTS, N_SP * CAP, D)
    gate_proj_grad, up_proj_grad, down_proj_grad, rows_grad = lax.map(
        expert_pass, (token_rows, grad_rows, gate_proj, up_proj, down_proj))
    picked = rows_grad.reshape(-1, D)[slot_index].reshape(TOKENS, TOP, D)
    token_grad = (cotangent.astype(jnp.float32) + jnp.sum(picked, axis=1)).astype(jnp.bfloat16)

    gate_f32 = gate_in.astype(jnp.float32)
    conv_f32 = conv_in.astype(jnp.float32)
    value_f32 = value_in.astype(jnp.float32)
    product = conv_f32 * value_f32
    padded = jnp.pad(product, ((1, 1), (0, 0)))
    conv_out = conv_taps[0] * padded[:-2] + conv_taps[1] * padded[1:-1] + conv_taps[2] * padded[2:]
    mixed_act = (gate_f32 * conv_out).astype(jnp.bfloat16)
    d_conv_out = jnp.dot(token_grad, out_weight, preferred_element_type=jnp.float32)
    gate_in_grad = (d_conv_out * conv_out).astype(jnp.bfloat16)
    back_signal = d_conv_out * gate_f32
    padded_back = jnp.pad(back_signal, ((1, 1), (0, 0)))
    d_product = conv_taps[0] * padded_back[2:] + conv_taps[1] * padded_back[1:-1] + conv_taps[2] * padded_back[:-2]
    conv_in_grad = (d_product * value_f32).astype(jnp.bfloat16)
    value_in_grad = (d_product * conv_f32).astype(jnp.bfloat16)
    out_weight_grad = jnp.dot(token_grad.T, mixed_act, preferred_element_type=jnp.float32)
    return (gate_proj_grad, up_proj_grad, down_proj_grad, out_weight_grad, token_grad,
            gate_in_grad, conv_in_grad, value_in_grad)
```

```python
import jax
import jax.numpy as jnp
from jax import lax
from jax.sharding import PartitionSpec as P

CLAMP_LIMIT = 7.0
SILU_ALPHA = 1.702


def contract_rows(left, right):
    return lax.dot_general(
        left, right, (((0,), (0,)), ((), ())), preferred_element_type=jnp.float32
    )


def contract_cols(left, right):
    return lax.dot_general(
        left, right, (((1,), (1,)), ((), ())), preferred_element_type=jnp.float32
    )


def halo(cells, axis):
    count = lax.axis_size(axis)
    ends = count - 1
    above = lax.ppermute(cells[-1:], axis, [(i, (i + 1) % count) for i in range(ends)])
    below = lax.ppermute(cells[:1], axis, [((i + 1) % count, i) for i in range(ends)])
    return jnp.concatenate([above, cells, below], axis=0)


def exchange_groups(partial_value, part_width):
    tp_count = lax.axis_size("tp")
    pairs = tp_count // 2
    me = lax.axis_index("tp")
    side, pair = me % 2, me // 2

    def block(which_pair, which_side):
        return lax.dynamic_slice_in_dim(
            partial_value, (2 * which_pair + which_side) * part_width, part_width, 1
        )

    others = [(i, i ^ 1) for i in range(tp_count)]
    sums = []
    for step in range(1, pairs + 1):
        target = (pair + step) % pairs
        given = block(target, 1 - side).astype(jnp.bfloat16)
        got = lax.ppermute(given, "tp", others)
        sums.append(block(target, side) + got.astype(jnp.float32))
    total = sums[-1]
    for step in range(1, pairs):
        moves = [(i, (i + 2 * step) % tp_count) for i in range(tp_count)]
        got = lax.ppermute(sums[step - 1].astype(jnp.bfloat16), "tp", moves)
        total = total + got.astype(jnp.float32)
    return total


def local(
    saved_tokens,
    cotangent,
    routes,
    route_weights,
    gate_in,
    conv_in,
    value_in,
    conv_taps,
    out_weight,
    gate_proj,
    up_proj,
    down_proj,
):
    tok_rows, model_width = saved_tokens.shape
    top_count = routes.shape[1]
    expert_count = lax.axis_size("sp")
    tp_count = lax.axis_size("tp")
    capacity = 2 * tok_rows * top_count // expert_count
    slots = expert_count * capacity
    part_width = model_width // tp_count
    channels = gate_in.shape[1]
    me_tp = lax.axis_index("tp")
    offset = me_tp * part_width

    routes_t = routes.T
    weights_t = route_weights.T
    experts = lax.broadcasted_iota(jnp.int32, (expert_count, tok_rows), 0)
    chosen = [experts == routes_t[k][None, :] for k in range(top_count)]
    hits = sum(c.astype(jnp.bfloat16) for c in chosen)
    earlier = (
        lax.broadcasted_iota(jnp.int32, (tok_rows, tok_rows), 0)
        < lax.broadcasted_iota(jnp.int32, (tok_rows, tok_rows), 1)
    ).astype(jnp.bfloat16)
    before = jnp.dot(hits, earlier, preferred_element_type=jnp.float32)
    slot_ids = lax.broadcasted_iota(jnp.int32, (slots, tok_rows), 0)
    place = jnp.zeros((slots, tok_rows), jnp.float32)
    weighted = jnp.zeros((slots, tok_rows), jnp.float32)
    for k in range(top_count):
        rank = jnp.sum(jnp.where(chosen[k], before, 0.0), axis=0).astype(jnp.int32)
        here = slot_ids == (routes_t[k] * capacity + rank)[None, :]
        place = jnp.where(here, 1.0, place)
        weighted = jnp.where(here, weights_t[k][None, :], weighted)
    place = place.astype(jnp.bfloat16)
    slot_weight = jnp.sum(weighted, axis=1, keepdims=True)

    own_tokens = lax.dynamic_slice_in_dim(saved_tokens, offset, part_width, 1)
    own_cot = lax.dynamic_slice_in_dim(cotangent, offset, part_width, 1)
    send_tokens = jnp.dot(place, own_tokens, preferred_element_type=jnp.float32).astype(jnp.bfloat16)
    cot_rows = jnp.dot(place, own_cot, preferred_element_type=jnp.float32)
    send_grads = (cot_rows * slot_weight).astype(jnp.bfloat16)

    def dispatched(rows):
        rows = rows.reshape(expert_count, capacity, part_width)
        return lax.all_to_all(rows, "sp", split_axis=0, concat_axis=0, tiled=True)

    arrived_tokens = dispatched(send_tokens)
    arrived_tokens, send_grads = lax.optimization_barrier((arrived_tokens, send_grads))
    arrived_grads = dispatched(send_grads)
    rows_in = lax.all_gather(arrived_tokens, "tp", axis=2, tiled=True).reshape(slots, model_width)
    grads_in = lax.all_gather(arrived_grads, "tp", axis=2, tiled=True).reshape(slots, model_width)

    gate_f32 = gate_in.astype(jnp.float32)
    conv_f32 = conv_in.astype(jnp.float32)
    value_f32 = value_in.astype(jnp.float32)
    my_taps = lax.dynamic_slice_in_dim(conv_taps, me_tp * channels, channels, 1)
    prod_rim = halo(conv_f32 * value_f32, "sp")
    conv_out = my_taps[0] * prod_rim[:-2] + my_taps[1] * prod_rim[1:-1] + my_taps[2] * prod_rim[2:]
    mixed = gate_f32 * conv_out

    w_gate, w_up, w_down = gate_proj[0], up_proj[0], down_proj[0]
    gate_pre = jnp.dot(rows_in, w_gate, preferred_element_type=jnp.float32)
    up_pre = jnp.dot(rows_in, w_up, preferred_element_type=jnp.float32)
    gate_clip = jnp.minimum(gate_pre, CLAMP_LIMIT)
    up_clip = jnp.clip(up_pre, -CLAMP_LIMIT, CLAMP_LIMIT)
    sigmoid_gate = jax.nn.sigmoid(SILU_ALPHA * gate_clip)
    gated_act = gate_clip * sigmoid_gate
    hidden = ((up_clip + 1.0) * gated_act).astype(jnp.bfloat16)
    grads_in, mixed = lax.optimization_barrier((grads_in, mixed))
    mixed_all = lax.all_gather(mixed, "sp", axis=0, tiled=True)
    d_hidden = contract_cols(grads_in, w_down)
    d_up = jnp.where(jnp.abs(up_pre) < CLAMP_LIMIT, d_hidden * gated_act, 0.0).astype(jnp.bfloat16)
    gate_slope = sigmoid_gate + SILU_ALPHA * gate_clip * sigmoid_gate * (1.0 - sigmoid_gate)
    d_gate = jnp.where(gate_pre < CLAMP_LIMIT, d_hidden * (up_clip + 1.0) * gate_slope, 0.0).astype(
        jnp.bfloat16
    )
    partial_value = contract_cols(d_gate, w_gate) + contract_cols(d_up, w_up)
    shares = exchange_groups(partial_value, part_width).astype(jnp.bfloat16)
    down_grad = contract_rows(hidden, grads_in)
    gate_grad = contract_rows(rows_in, d_gate)
    up_grad = contract_rows(rows_in, d_up)

    returned = dispatched(shares).reshape(slots, part_width)
    combined = contract_rows(place, returned)
    token_grad = (own_cot.astype(jnp.float32) + combined).astype(jnp.bfloat16)
    residual = lax.all_gather(token_grad, "tp", axis=1, tiled=True)

    d_conv_out = jnp.dot(residual, out_weight, preferred_element_type=jnp.float32)
    grad_rim = halo(d_conv_out * gate_f32, "sp")
    d_product = my_taps[0] * grad_rim[2:] + my_taps[1] * grad_rim[1:-1] + my_taps[2] * grad_rim[:-2]
    gate_in_grad = (d_conv_out * conv_out).astype(jnp.bfloat16)
    conv_in_grad = (d_product * value_f32).astype(jnp.bfloat16)
    value_in_grad = (d_product * conv_f32).astype(jnp.bfloat16)

    share = tok_rows // tp_count
    quarter = lax.dynamic_slice_in_dim(residual, me_tp * share, share, 0)
    quarter = quarter.reshape(share, expert_count, model_width // expert_count)
    quarter = lax.all_to_all(
        quarter.transpose(1, 0, 2), "sp", split_axis=0, concat_axis=0, tiled=True
    )
    features = lax.all_gather(quarter, "tp", axis=1, tiled=True)
    features = features.reshape(expert_count * tok_rows, -1)
    mixed_all = lax.optimization_barrier(mixed_all).astype(jnp.bfloat16)
    out_weight_grad = contract_rows(features, mixed_all)
    return (
        gate_grad[None],
        up_grad[None],
        down_grad[None],
        out_weight_grad,
        token_grad,
        gate_in_grad,
        conv_in_grad,
        value_in_grad,
    )


def solution(mesh):
    in_specs = (
        P("sp", None),
        P("sp", None),
        P("sp", None),
        P("sp", None),
        P("sp", "tp"),
        P("sp", "tp"),
        P("sp", "tp"),
        P(),
        P(None, "tp"),
        P("sp", None, "tp"),
        P("sp", None, "tp"),
        P("sp", "tp", None),
    )
    out_specs = (
        P("sp", None, "tp"),
        P("sp", None, "tp"),
        P("sp", "tp", None),
        P("sp", "tp"),
        P("sp", "tp"),
        P("sp", "tp"),
        P("sp", "tp"),
        P("sp", "tp"),
    )
    return jax.shard_map(local, mesh=mesh, in_specs=in_specs, out_specs=out_specs, check_vma=False)
```

```python
import jax
import jax.numpy as jnp
from jax import lax
from jax.sharding import PartitionSpec as P

CLAMP_LIMIT = 7.0
SILU_ALPHA = 1.702


def contract_rows(left, right):
    return lax.dot_general(
        left, right, (((0,), (0,)), ((), ())), preferred_element_type=jnp.float32
    )


def contract_cols(left, right):
    return lax.dot_general(
        left, right, (((1,), (1,)), ((), ())), preferred_element_type=jnp.float32
    )


def halo(cells, axis):
    count = lax.axis_size(axis)
    ends = count - 1
    above = lax.ppermute(cells[-1:], axis, [(i, (i + 1) % count) for i in range(ends)])
    below = lax.ppermute(cells[:1], axis, [((i + 1) % count, i) for i in range(ends)])
    return jnp.concatenate([above, cells, below], axis=0)


def exchange_groups(partial_value, part_width):
    tp_count = lax.axis_size("tp")
    pairs = tp_count // 2
    me = lax.axis_index("tp")
    side, pair = me % 2, me // 2

    def block(which_pair, which_side):
        return lax.dynamic_slice_in_dim(
            partial_value, (2 * which_pair + which_side) * part_width, part_width, 1
        )

    others = [(i, i ^ 1) for i in range(tp_count)]
    sums = []
    for step in range(1, pairs + 1):
        target = (pair + step) % pairs
        given = block(target, 1 - side).astype(jnp.bfloat16)
        got = lax.ppermute(given, "tp", others)
        sums.append(block(target, side) + got.astype(jnp.float32))
    total = sums[-1]
    for step in range(1, pairs):
        moves = [(i, (i + 2 * step) % tp_count) for i in range(tp_count)]
        got = lax.ppermute(sums[step - 1].astype(jnp.bfloat16), "tp", moves)
        total = total + got.astype(jnp.float32)
    return total


def gather_features(part):
    tp_count = lax.axis_size("tp")
    pairs = tp_count // 2
    me = lax.axis_index("tp")
    side, pair = me % 2, me // 2
    width = part.shape[1]
    others = [(i, i ^ 1) for i in range(tp_count)]
    held = [part]
    for step in range(1, pairs):
        moves = [(i, (i + 2 * step) % tp_count) for i in range(tp_count)]
        held.append(lax.ppermute(part, "tp", moves))
    twins = [lax.ppermute(block, "tp", others) for block in held]
    whole = jnp.zeros((part.shape[0], tp_count * width), part.dtype)
    for step in range(pairs):
        first = 2 * ((pair - step) % pairs)
        whole = lax.dynamic_update_slice_in_dim(whole, held[step], (first + side) * width, 1)
        whole = lax.dynamic_update_slice_in_dim(whole, twins[step], (first + 1 - side) * width, 1)
    return whole


def local(
    saved_tokens,
    cotangent,
    routes,
    route_weights,
    gate_in,
    conv_in,
    value_in,
    conv_taps,
    out_weight,
    gate_proj,
    up_proj,
    down_proj,
):
    tok_rows, model_width = saved_tokens.shape
    top_count = routes.shape[1]
    expert_count = lax.axis_size("sp")
    tp_count = lax.axis_size("tp")
    capacity = 2 * tok_rows * top_count // expert_count
    slots = expert_count * capacity
    part_width = model_width // tp_count
    channels = gate_in.shape[1]
    me_tp = lax.axis_index("tp")
    offset = me_tp * part_width

    routes_t = routes.T
    weights_t = route_weights.T
    experts = lax.broadcasted_iota(jnp.int32, (expert_count, tok_rows), 0)
    chosen = [experts == routes_t[k][None, :] for k in range(top_count)]
    hits = sum(c.astype(jnp.bfloat16) for c in chosen)
    earlier = (
        lax.broadcasted_iota(jnp.int32, (tok_rows, tok_rows), 0)
        < lax.broadcasted_iota(jnp.int32, (tok_rows, tok_rows), 1)
    ).astype(jnp.bfloat16)
    before = jnp.dot(hits, earlier, preferred_element_type=jnp.float32)
    slot_ids = lax.broadcasted_iota(jnp.int32, (slots, tok_rows), 0)
    place = jnp.zeros((slots, tok_rows), jnp.float32)
    weighted = jnp.zeros((slots, tok_rows), jnp.float32)
    for k in range(top_count):
        rank = jnp.sum(jnp.where(chosen[k], before, 0.0), axis=0).astype(jnp.int32)
        here = slot_ids == (routes_t[k] * capacity + rank)[None, :]
        place = jnp.where(here, 1.0, place)
        weighted = jnp.where(here, weights_t[k][None, :], weighted)
    place = place.astype(jnp.bfloat16)
    slot_weight = jnp.sum(weighted, axis=1, keepdims=True)

    own_tokens = lax.dynamic_slice_in_dim(saved_tokens, offset, part_width, 1)
    own_cot = lax.dynamic_slice_in_dim(cotangent, offset, part_width, 1)
    send_tokens = jnp.dot(place, own_tokens, preferred_element_type=jnp.float32).astype(jnp.bfloat16)
    cot_rows = jnp.dot(place, own_cot, preferred_element_type=jnp.float32)
    send_grads = (cot_rows * slot_weight).astype(jnp.bfloat16)

    def dispatched(rows):
        rows = rows.reshape(expert_count, capacity, part_width)
        return lax.all_to_all(rows, "sp", split_axis=0, concat_axis=0, tiled=True)

    arrived_tokens = dispatched(send_tokens)
    arrived_tokens, send_grads = lax.optimization_barrier((arrived_tokens, send_grads))
    arrived_grads = dispatched(send_grads)
    rows_in = gather_features(arrived_tokens.reshape(slots, part_width))
    grads_in = gather_features(arrived_grads.reshape(slots, part_width))

    gate_f32 = gate_in.astype(jnp.float32)
    conv_f32 = conv_in.astype(jnp.float32)
    value_f32 = value_in.astype(jnp.float32)
    my_taps = lax.dynamic_slice_in_dim(conv_taps, me_tp * channels, channels, 1)
    prod_rim = halo(conv_f32 * value_f32, "sp")
    conv_out = my_taps[0] * prod_rim[:-2] + my_taps[1] * prod_rim[1:-1] + my_taps[2] * prod_rim[2:]
    mixed = (gate_f32 * conv_out).astype(jnp.bfloat16)
    mixed = jnp.concatenate([mixed, mixed], axis=1)

    w_gate, w_up, w_down = gate_proj[0], up_proj[0], down_proj[0]
    gate_pre = jnp.dot(rows_in, w_gate, preferred_element_type=jnp.float32)
    up_pre = jnp.dot(rows_in, w_up, preferred_element_type=jnp.float32)
    gate_clip = jnp.minimum(gate_pre, CLAMP_LIMIT)
    up_clip = jnp.clip(up_pre, -CLAMP_LIMIT, CLAMP_LIMIT)
    sigmoid_gate = jax.nn.sigmoid(SILU_ALPHA * gate_clip)
    gated_act = gate_clip * sigmoid_gate
    hidden = ((up_clip + 1.0) * gated_act).astype(jnp.bfloat16)
    grads_in, mixed = lax.optimization_barrier((grads_in, mixed))
    mixed_all = lax.all_gather(mixed, "sp", axis=0, tiled=True)
    d_hidden = contract_cols(grads_in, w_down)
    d_up = jnp.where(jnp.abs(up_pre) < CLAMP_LIMIT, d_hidden * gated_act, 0.0).astype(jnp.bfloat16)
    gate_slope = sigmoid_gate + SILU_ALPHA * gate_clip * sigmoid_gate * (1.0 - sigmoid_gate)
    d_gate = jnp.where(gate_pre < CLAMP_LIMIT, d_hidden * (up_clip + 1.0) * gate_slope, 0.0).astype(
        jnp.bfloat16
    )
    partial_value = contract_cols(d_gate, w_gate) + contract_cols(d_up, w_up)
    shares = exchange_groups(partial_value, part_width).astype(jnp.bfloat16)
    down_grad = contract_rows(hidden, grads_in)
    gate_grad = contract_rows(rows_in, d_gate)
    up_grad = contract_rows(rows_in, d_up)

    returned = dispatched(shares).reshape(slots, part_width)
    combined = contract_rows(place, returned)
    token_grad = (own_cot.astype(jnp.float32) + combined).astype(jnp.bfloat16)
    residual = lax.all_gather(token_grad, "tp", axis=1, tiled=True)

    d_conv_out = jnp.dot(residual, out_weight, preferred_element_type=jnp.float32)
    grad_rim = halo(d_conv_out * gate_f32, "sp")
    d_product = my_taps[0] * grad_rim[2:] + my_taps[1] * grad_rim[1:-1] + my_taps[2] * grad_rim[:-2]
    gate_in_grad = (d_conv_out * conv_out).astype(jnp.bfloat16)
    conv_in_grad = (d_product * value_f32).astype(jnp.bfloat16)
    value_in_grad = (d_product * conv_f32).astype(jnp.bfloat16)

    share = tok_rows // tp_count
    quarter = lax.dynamic_slice_in_dim(residual, me_tp * share, share, 0)
    quarter = quarter.reshape(share, expert_count, model_width // expert_count)
    quarter = lax.all_to_all(
        quarter.transpose(1, 0, 2), "sp", split_axis=0, concat_axis=0, tiled=True
    )
    features = lax.all_gather(quarter, "tp", axis=1, tiled=True)
    features = features.reshape(expert_count * tok_rows, -1)
    out_weight_grad = contract_rows(features, mixed_all[:, :channels])
    return (
        gate_grad[None],
        up_grad[None],
        down_grad[None],
        out_weight_grad,
        token_grad,
        gate_in_grad,
        conv_in_grad,
        value_in_grad,
    )


def solution(mesh):
    in_specs = (
        P("sp", None),
        P("sp", None),
        P("sp", None),
        P("sp", None),
        P("sp", "tp"),
        P("sp", "tp"),
        P("sp", "tp"),
        P(),
        P(None, "tp"),
        P("sp", None, "tp"),
        P("sp", None, "tp"),
        P("sp", "tp", None),
    )
    out_specs = (
        P("sp", None, "tp"),
        P("sp", None, "tp"),
        P("sp", "tp", None),
        P("sp", "tp"),
        P("sp", "tp"),
        P("sp", "tp"),
        P("sp", "tp"),
        P("sp", "tp"),
    )
    return jax.shard_map(local, mesh=mesh, in_specs=in_specs, out_specs=out_specs, check_vma=False)
```
